256 devices in a mesh: ra: 32 (over z, y), cb: 8 (over x, core).
Axes of the slice: x: 4, y: 4, z: 8, core: 2. Of those that a mesh axis runs over, the one named last changes fastest.
Arguments:
- tokens: bfloat16 [2048, 16384], P('ra'), may hold values from -16 to 16
- norm_gain: float32 [2, 2048], replicated, may hold values from 0.1 to 1.9
- up_weight: float32 [2, 2048, 6144], P(None, 'ra', 'cb'), may hold values from -0.125 to 0.125
- gate_weight: float32 [2, 2048, 6144], P(None, 'ra', 'cb'), may hold values from -0.125 to 0.125
- up_scale: float32 [2, 6144], P(None, 'cb'), may hold values from 0.5 to 2
- gate_scale: float32 [2, 6144], P(None, 'cb'), may hold values from 0.5 to 2
- up_taps: float32 [2, 3, 6144], P(None, None, 'cb'), may hold values from -3 to 3
- gate_taps: float32 [2, 3, 6144], P(None, None, 'cb'), may hold values from -3 to 3
- down_weight: float32 [2, 2048, 6144], P(None, 'ra', 'cb'), may hold values from -0.078125 to 0.078125
- down_scale: float32 [2, 2048], replicated, may hold values from 0.5 to 2
Outputs:
- mixed: bfloat16 [2048, 16384], P('ra')
The draws below stay inside these ranges and needn't reach their ends.
All inputs are finite; a program needn't handle non-finite values.
Results may differ from the reference program's by a relative error of at most 0.024.
Values may be sent and summed in bfloat16 or wider, within the bound.
No kernel may reach another device: no remote copies, remote signals or barrier semaphores. Data moves between devices by JAX's collectives and lax.ppermute only.
A program may use at most 64 MiB of HBM per device.

```python
import math
import jax
import jax.numpy as jnp
from jax import lax

D = 2048
FF = 6144
KW = 3
LAYERS = 2
TOKENS = 16384
N_RA = 32
N_CB = 8


def draw_tokens(key, part):
    first, second, third = jax.random.split(key, 3)
    blocks = jnp.exp(jax.random.uniform(second, (N_RA,), jnp.float32, math.log(0.3), math.log(3.0)))
    features = jnp.repeat(blocks, D // N_RA, total_repeat_length=D)
    base = jnp.clip(jax.random.normal(first, (D, TOKENS), jnp.float32), -4.0, 4.0)
    return (base * features[:, None]).astype(jnp.bfloat16)


def shard_levels(rng, extent, cuts, smallest, high):
    gain, own = 1.0, jax.random.fold_in(rng, 6)
    for position, parts in cuts:
        draws = jnp.exp(jax.random.uniform(jax.random.fold_in(own, position), (parts,), jnp.float32, smallest / len(cuts), high / len(cuts)))
        gain = gain * jnp.repeat(draws, extent[position] // parts).reshape([-1 if axis == position else 1 for axis in range(len(extent))])
    return gain


def normal_values(stream_key, extent, scale, bound, pieces=(), dtype=jnp.bfloat16):
    level = shard_levels(stream_key, extent, pieces, -0.22, 0.18) if pieces else 1.0
    values = jax.random.normal(stream_key, extent, jnp.float32) * scale * level
    return jnp.minimum(jnp.maximum(values, -bound), bound).astype(dtype)


def setup_inputs(seed: int = 0) -> dict:
    splits = jax.random.split(jax.random.key(seed), 11)
    return {
        "tokens": draw_tokens(jax.random.fold_in(splits[10], 71), 0),
        "norm_gain": jnp.clip(1.0 + 0.18 * jax.random.normal(splits[1], (LAYERS, D), jnp.float32), 0.1, 1.9),
        "up_weight": normal_values(splits[2], (LAYERS, D, FF), D ** -0.5, 0.125, ((1, 32), (2, 8)), jnp.float32),
        "gate_weight": normal_values(splits[3], (LAYERS, D, FF), D ** -0.5, 0.125, ((1, 32), (2, 8)), jnp.float32),
        "up_scale": jnp.clip(jnp.exp(math.log(2.0) - 1.3862944 * jax.random.uniform(splits[4], (LAYERS, FF), jnp.float32) ** shard_levels(splits[4], (LAYERS, FF), ((1, 8),), -0.2, 0.2)), 0.5, 2.0),
        "gate_scale": jnp.clip(jnp.exp(math.log(2.0) - 1.3862944 * jax.random.uniform(splits[5], (LAYERS, FF), jnp.float32) ** shard_levels(splits[5], (LAYERS, FF), ((1, 8),), -0.2, 0.2)), 0.5, 2.0),
        "up_taps": normal_values(splits[6], (LAYERS, KW, FF), 0.6, 3.0, ((2, 8),), jnp.float32),
        "gate_taps": normal_values(splits[7], (LAYERS, KW, FF), 0.6, 3.0, ((2, 8),), jnp.float32),
        "down_weight": normal_values(splits[8], (LAYERS, D, FF), FF ** -0.5, 0.078125, ((1, 32), (2, 8)), jnp.float32),
        "down_scale": jnp.clip(jnp.exp(jax.random.uniform(splits[9], (LAYERS, D), jnp.float32, math.log(0.5), math.log(2.0))), 0.5, 2.0),
    }


EPS = 1e-06
RESIDUAL = 0.5

def causal_taps(values, taps):
    width = taps.shape[0]
    length = values.shape[0]
    padded = jnp.pad(values, ((width - 1, 0), (0, 0)))
    total = jnp.zeros_like(values)
    for k in range(width):
        total = total + taps[k][None, :] * padded[k:k + length]
    return total

def reference(tokens, norm_gain, up_weight, gate_weight, up_scale, gate_scale, up_taps, gate_taps, down_weight, down_scale):
    state = tokens.T
    block = FF // N_CB
    for layer in range(LAYERS):
        state_f = state.astype(jnp.float32)
        inverse = lax.rsqrt(lax.optimization_barrier(jnp.mean(state_f * state_f, axis=1, keepdims=True)) + EPS)
        scaled = (state_f * norm_gain[layer][None, :]).astype(jnp.bfloat16)
        up_raw = jnp.dot(scaled, up_weight[layer].astype(jnp.bfloat16), preferred_element_type=jnp.float32)
        gate_raw = jnp.dot(scaled, gate_weight[layer].astype(jnp.bfloat16), preferred_element_type=jnp.float32)
        up_pre = up_raw * inverse * up_scale[layer][None, :]
        gate_pre = gate_raw * inverse * gate_scale[layer][None, :]
        conv_up = causal_taps(up_pre, up_taps[layer])
        conv_gate = causal_taps(gate_pre, gate_taps[layer])
        hidden = (jax.nn.silu(conv_gate) * conv_up).astype(jnp.bfloat16)
        weight_b = down_weight[layer].astype(jnp.bfloat16)
        down = jnp.zeros((hidden.shape[0], weight_b.shape[0]), jnp.float32)
        for group in range(N_CB):
            term = jnp.dot(hidden[:, group * block:(group + 1) * block], weight_b[:, group * block:(group + 1) * block].T, preferred_element_type=jnp.float32)
            rounded = lax.optimization_barrier(term.astype(jnp.bfloat16))
            down = down + rounded.astype(jnp.float32)
        state = (down * down_scale[layer][None, :] + RESIDUAL * state_f).astype(jnp.bfloat16)
    return state.T
```

```python
import jax
import jax.numpy as jnp
from jax import lax
from jax.sharding import Mesh
from jax.sharding import PartitionSpec as P

RA = ("z", "y")
CB = ("x", "c")
EPS = 1e-06
RESIDUAL = 0.5
BF = jnp.bfloat16
F32 = jnp.float32


def turned(value, axis, steps):
    count = lax.axis_size(axis)
    return lax.ppermute(value, axis, [(s, (s + steps) % count) for s in range(count)])


def shifted(value, axis, steps):
    count = lax.axis_size(axis)
    initial, last = (max(0, -steps), min(count, count - steps))
    return lax.ppermute(value, axis, [(s, s + steps) for s in range(initial, last)])


def at(blocks, index):
    return lax.dynamic_index_in_dim(blocks, index, 0, keepdims=False)


def gather_cb(own):
    half = own.shape[0] // 2
    x = lax.axis_index("x")
    c = lax.axis_index("c")
    left = turned(own, "x", 1)
    right = turned(own, "x", -1)
    far_low = turned(left[:half], "x", 1)
    far_high = turned(right[half:], "x", -1)
    far = jnp.concatenate([far_low, far_high], axis=0)
    whole = jnp.zeros((4, *own.shape), own.dtype)
    for steps, block in ((0, own), (3, left), (1, right), (2, far)):
        whole = lax.dynamic_update_index_in_dim(whole, block, (x + steps) % 4, 0)
    other = turned(whole, "c", 1)
    first = jnp.where(c == 0, whole, other)
    second = jnp.where(c == 0, other, whole)
    return jnp.stack([first, second], axis=1)


def scatter_cb(parts):
    x = lax.axis_index("x")
    c = lax.axis_index("c")
    mine = jnp.where(c == 0, parts[:, 0], parts[:, 1])
    sent = jnp.where(c == 0, parts[:, 1], parts[:, 0])
    pair = (mine.astype(F32) + turned(sent, "c", 1).astype(F32)).astype(BF)
    half = pair.shape[1] // 2
    far = at(pair, (x + 2) % 4)
    from_left = turned(far[:half], "x", 1)
    from_right = turned(far[half:], "x", -1)
    to_right = at(pair, (x + 1) % 4)
    to_left = at(pair, (x + 3) % 4)
    low = (to_right[:half].astype(F32) + from_left.astype(F32)).astype(BF)
    high = (to_left[half:].astype(F32) + from_right.astype(F32)).astype(BF)
    a = turned(jnp.concatenate([low, to_right[half:]], axis=0), "x", 1)
    b = turned(jnp.concatenate([to_left[:half], high], axis=0), "x", -1)
    return at(pair, x).astype(F32) + a.astype(F32) + b.astype(F32)


def valid_taps(values, taps):
    width = taps.shape[0]
    length = values.shape[0] - width + 1
    total = taps[0][None, :] * values[0:length]
    for k in range(1, width):
        total = total + taps[k][None, :] * values[k : k + length]
    return total


def per_device(
    tokens,
    norm_gain,
    up_weight,
    gate_weight,
    up_scale,
    gate_scale,
    up_taps,
    gate_taps,
    down_weight,
    down_scale,
):
    layers = up_weight.shape[0]
    ra = lax.axis_size("z") * lax.axis_size("y")
    cb = lax.axis_index("x") * 2 + lax.axis_index("c")
    rows, hid = up_weight.shape[1:]
    width = rows * ra
    part = rows // 8
    span = tokens.shape[1] // ra

    shards = [
        jnp.concatenate([w[l].astype(BF) for w in (up_weight, gate_weight, down_weight)], axis=1)
        for l in range(layers)
    ]
    weights = [lax.all_gather(s, RA, axis=0, tiled=True) for s in shards]

    own = lax.dynamic_slice_in_dim(tokens, cb * part, part, 0)
    own = own.reshape(part, ra, span).transpose(1, 0, 2)
    own = lax.all_to_all(own, RA, split_axis=0, concat_axis=0, tiled=True)
    every = gather_cb(own)
    state = every.reshape(8, ra, part, span).transpose(3, 1, 0, 2).reshape(span, width)

    edge = up_taps.shape[1] - 1
    for l in range(layers):
        before = shifted(state[span - edge :], RA, 1)
        rows_all = jnp.concatenate([before, state], axis=0)
        rows_f = rows_all.astype(F32)
        inverse = lax.rsqrt(jnp.mean(rows_f * rows_f, axis=1, keepdims=True) + EPS)
        scaled = (rows_f * norm_gain[l][None, :]).astype(BF)
        w = weights[l]
        up_raw = jnp.dot(scaled, w[:, :hid], preferred_element_type=F32)
        gate_raw = jnp.dot(scaled, w[:, hid : 2 * hid], preferred_element_type=F32)
        conv_up = valid_taps(up_raw * inverse * up_scale[l][None, :], up_taps[l])
        conv_gate = valid_taps(gate_raw * inverse * gate_scale[l][None, :], gate_taps[l])
        hidden = (jax.nn.silu(conv_gate) * conv_up).astype(BF)
        down_w = w[:, 2 * hid :]
        if l + 1 < layers:
            down = lax.dot_general(
                hidden, down_w, (((1,), (1,)), ((), ())), preferred_element_type=F32
            ).astype(BF)
            piece = scatter_cb(down.reshape(4, 2, span // 8, width))
            held = lax.dynamic_slice_in_dim(state, cb * (span // 8), span // 8, 0)
            piece = (piece * down_scale[l][None, :] + RESIDUAL * held.astype(F32)).astype(BF)
            state = gather_cb(piece).reshape(span, width)
        else:
            down = lax.dot_general(
                down_w, hidden, (((1,), (1,)), ((), ())), preferred_element_type=F32
            ).astype(BF)
            down = down.reshape(ra, 4, 2, part, span).transpose(1, 2, 0, 3, 4)
            piece = scatter_cb(down)
            held = lax.dynamic_index_in_dim(
                state.reshape(span, ra, 8, part), cb, 2, keepdims=False
            ).transpose(1, 2, 0)
            scale = lax.dynamic_index_in_dim(
                down_scale[l].reshape(ra, 8, part), cb, 1, keepdims=False
            )
            piece = (piece * scale[:, :, None] + RESIDUAL * held.astype(F32)).astype(BF)
    piece = lax.all_to_all(piece, RA, split_axis=0, concat_axis=0, tiled=True)
    piece = piece.transpose(1, 0, 2).reshape(part, ra * span)
    return gather_cb(piece).reshape(rows, ra * span)


def solution(mesh):
    torus = Mesh(mesh.devices.reshape(8, 4, 4, 2), ("z", "y", "x", "c"))
    placed = (
        P(RA, None),
        P(),
        P(None, RA, CB),
        P(None, RA, CB),
        P(None, CB),
        P(None, CB),
        P(None, None, CB),
        P(None, None, CB),
        P(None, RA, CB),
        P(),
    )
    return jax.shard_map(
        per_device, mesh=torus, in_specs=placed, out_specs=P(RA, None), check_vma=False
    )
```

```python
import jax
import jax.numpy as jnp
from jax import lax
from jax.sharding import Mesh
from jax.sharding import PartitionSpec as P

RA = ("z", "y")
CB = ("x", "c")
EPS = 1e-06
RESIDUAL = 0.5
BF = jnp.bfloat16
F32 = jnp.float32


def turned(value, axis, steps):
    count = lax.axis_size(axis)
    return lax.ppermute(value, axis, [(s, (s + steps) % count) for s in range(count)])


def shifted(value, axis, steps):
    count = lax.axis_size(axis)
    initial, last = (max(0, -steps), min(count, count - steps))
    return lax.ppermute(value, axis, [(s, s + steps) for s in range(initial, last)])


def at(blocks, index):
    return lax.dynamic_index_in_dim(blocks, index, 0, keepdims=False)


def ring(own, axis):
    count = lax.axis_size(axis)
    half = own.shape[0] // 2
    found = [(0, 0, own)]
    low, high = own, own
    for k in range(1, count // 2):
        low, high = turned(low, axis, 1), turned(high, axis, -1)
        found += [(count - k, 0, low), (k, 0, high)]
    far = count // 2
    found += [(far, 0, turned(low[:half], axis, 1)), (far, half, turned(high[half:], axis, -1))]
    return found


def placed_in(whole, found, axis, size, start):
    index = lax.axis_index(axis)
    count = lax.axis_size(axis)
    for back, first, block in found:
        whole = lax.dynamic_update_slice_in_dim(
            whole, block, start + (index + back) % count * size + first, 0
        )
    return whole


def joined(found, axis):
    size = found[0][2].shape[0]
    count = lax.axis_size(axis)
    whole = lax.optimization_barrier(jnp.zeros((count * size, found[0][2].shape[1]), BF))
    return placed_in(whole, found, axis, size, 0)


def gather_rows(own):
    rows, cols = own.shape
    half = rows // 2
    nz, ny = lax.axis_size("z"), lax.axis_size("y")
    second = joined(ring(own[half:], "y"), "y")
    first = joined(ring(own[:half], "z"), "z")
    by_z = ring(second, "z")
    by_y = ring(first, "y")
    na, nb = nz * half, ny * half
    start = na * ny
    whole = lax.optimization_barrier(jnp.zeros((rows * nz * ny, cols), BF))
    whole = placed_in(whole, by_z[:1], "z", nb, start)
    whole = placed_in(whole, by_y[:1], "y", na, 0)
    whole = placed_in(whole, by_z[1:3], "z", nb, start)
    whole = placed_in(whole, by_y[1:3], "y", na, 0)
    whole = placed_in(whole, by_z[3:-2], "z", nb, start)
    whole = placed_in(whole, by_y[3:], "y", na, 0)
    return placed_in(whole, by_z[-2:], "z", nb, start)


def gather_cb(own):
    x = lax.axis_index("x")
    blocks = ((0, own), (3, turned(own, "x", 1)), (1, turned(own, "x", -1)), (2, turned(own, "x", 2)))
    whole = jnp.zeros((4, *own.shape), own.dtype)
    for back, block in blocks:
        whole = lax.dynamic_update_index_in_dim(whole, block, (x + back) % 4, 0)
    other = turned(whole, "c", 1)
    zero = lax.axis_index("c") == 0
    return jnp.where(zero, whole, other), jnp.where(zero, other, whole)


def scatter_cb(first, second):
    x = lax.axis_index("x")
    zero = lax.axis_index("c") == 0
    kept = jnp.where(zero, first, second)
    got = turned(jnp.where(zero, second, first), "c", 1)

    def pair(k):
        return at(kept, (x + k) % 4).astype(F32) + at(got, (x + k) % 4).astype(F32)

    sums = [turned(pair(k).astype(BF), "x", k) for k in (1, 3, 2)]
    total = pair(0)
    for s in sums:
        total = total + s.astype(F32)
    return total


def taps_of(values, before, taps):
    edge = before.shape[0]
    rows = jnp.concatenate([before, values], axis=0)
    total = taps[edge][None, :] * values
    for k in range(edge):
        total = total + taps[k][None, :] * rows[k : k + values.shape[0]]
    return total


def hidden_of(state, gain, w, hid, up_scale, gate_scale, up_taps, gate_taps):
    state_f = state.astype(F32)
    inverse = lax.rsqrt(jnp.mean(state_f * state_f, axis=0) + EPS)[:, None]
    scaled = (state_f * gain[:, None]).astype(BF)

    def product(first):
        return lax.dot_general(
            scaled, w[:, first : first + hid], (((0,), (0,)), ((), ())), preferred_element_type=F32
        )

    up = product(0) * inverse * up_scale[None, :]
    gate = product(hid) * inverse * gate_scale[None, :]
    edge = up_taps.shape[0] - 1
    before = shifted(jnp.concatenate([up[-edge:], gate[-edge:]], axis=0), RA, 1)
    conv_up = taps_of(up, before[:edge], up_taps)
    conv_gate = taps_of(gate, before[edge:], gate_taps)
    return (jax.nn.silu(conv_gate) * conv_up).astype(BF)


def down_of(w, hidden):
    return lax.dot_general(w, hidden, (((1,), (1,)), ((), ())), preferred_element_type=F32).astype(BF)


def split_order(values):
    v = values.reshape(8, 4, 2, 32, *values.shape[1:])
    first = jnp.swapaxes(v[:, :, 0], 0, 1).reshape(1024, *values.shape[1:])
    return jnp.concatenate([first, v[:, :, 1].reshape(1024, *values.shape[1:])], axis=0)


def per_device(
    tokens,
    norm_gain,
    up_weight,
    gate_weight,
    up_scale,
    gate_scale,
    up_taps,
    gate_taps,
    down_weight,
    down_scale,
):
    rows, hid = up_weight.shape[1:]
    ra = lax.axis_size(RA)
    x, c = lax.axis_index("x"), lax.axis_index("c")
    cb = x * 2 + c
    part = rows // 8
    span = tokens.shape[1] // ra
    width = rows * ra

    shards = [
        jnp.concatenate([w[l].astype(BF) for w in (up_weight, gate_weight, down_weight)], axis=1)
        for l in range(2)
    ]
    w0 = gather_rows(shards[0])
    w1 = lax.all_gather(shards[1], RA, axis=0, tiled=True)

    own = lax.dynamic_slice_in_dim(tokens, cb * part, part, 0)
    own = own.reshape(part, ra, span).transpose(1, 0, 2)
    own = lax.all_to_all(own, RA, split_axis=0, concat_axis=0, tiled=True)
    even, odd = gather_cb(own.reshape(ra * part, span))
    every = jnp.stack([even, odd], axis=1).reshape(2, 4, 8, 4, part, span)
    state = jnp.concatenate(
        [
            every[0].transpose(2, 1, 0, 3, 4).reshape(width // 2, span),
            every[1].transpose(1, 2, 0, 3, 4).reshape(width // 2, span),
        ],
        axis=0,
    )

    def hidden(l, state, gain, w):
        return hidden_of(
            state, gain, w, hid, up_scale[l], gate_scale[l], up_taps[l], gate_taps[l]
        )

    h = hidden(0, state, split_order(norm_gain[0]), w0)
    down_w = w0[:, 2 * hid :]
    block = width // 8
    sums = scatter_cb(
        down_of(down_w[: width // 2], h).reshape(4, block, span),
        down_of(down_w[width // 2 :], h).reshape(4, block, span),
    )
    place = (c * 4 + x) * block
    held = lax.dynamic_slice_in_dim(state, place, block, 0)
    scale = lax.dynamic_slice_in_dim(split_order(down_scale[0]), place, block, 0)
    piece = (sums * scale[:, None] + RESIDUAL * held.astype(F32)).astype(BF)
    first, second = gather_cb(piece)
    state = jnp.stack(
        [
            first.reshape(4, 8, rows // 2, span).transpose(1, 0, 2, 3),
            second.reshape(8, 4, rows // 2, span),
        ],
        axis=2,
    ).reshape(width, span)

    h = hidden(1, state, norm_gain[1], w1)
    down = down_of(w1[:, 2 * hid :], h).reshape(ra, 4, 2, part, span)
    sums = scatter_cb(
        *(down[:, :, k].transpose(1, 0, 2, 3).reshape(4, block, span) for k in range(2))
    )
    held = lax.dynamic_index_in_dim(state.reshape(ra, 8, part, span), cb, 1, keepdims=False)
    scale = lax.dynamic_index_in_dim(down_scale[1].reshape(ra, 8, part), cb, 1, keepdims=False)
    piece = sums.reshape(ra, part, span) * scale[:, :, None] + RESIDUAL * held.astype(F32)
    piece = lax.all_to_all(piece.astype(BF), RA, split_axis=0, concat_axis=0, tiled=True)
    piece = piece.transpose(1, 0, 2).reshape(part, ra * span)
    even, odd = gather_cb(piece)
    return jnp.stack([even, odd], axis=1).reshape(rows, ra * span)


def solution(mesh):
    torus = Mesh(mesh.devices.reshape(8, 4, 4, 2), ("z", "y", "x", "c"))
    placed = (
        P(RA, None),
        P(),
        P(None, RA, CB),
        P(None, RA, CB),
        P(None, CB),
        P(None, CB),
        P(None, None, CB),
        P(None, None, CB),
        P(None, RA, CB),
        P(),
    )
    return jax.shard_map(
        per_device, mesh=torus, in_specs=placed, out_specs=P(RA, None), check_vma=False
    )
```

```python
import jax
import jax.numpy as jnp
from jax import lax
from jax.experimental import pallas as pl
from jax.experimental.pallas import tpu as pltpu
from jax.sharding import Mesh
from jax.sharding import PartitionSpec as P


RA = ("z", "y")
CB = ("x", "c")
NZ, NY, NX, NC = 8, 4, 4, 2
AHEAD = 128
EPS = 1e-06
RESIDUAL = 0.5
BF = jnp.bfloat16
F32 = jnp.float32
HBM = pl.BlockSpec(memory_space=pltpu.HBM)
SMEM = pl.BlockSpec(memory_space=pltpu.SMEM)
VMEM = pl.BlockSpec(memory_space=pltpu.VMEM)


def turned(value, axis, steps):
    count = lax.axis_size(axis)
    return lax.ppermute(value, axis, [(s, (s + steps) % count) for s in range(count)])


def shifted(value, axis, steps):
    count = lax.axis_size(axis)
    initial, last = (max(0, -steps), min(count, count - steps))
    return lax.ppermute(value, axis, [(s, s + steps) for s in range(initial, last)])


def after(value, *others):
    return lax.optimization_barrier((value, *others))[0]


def ring(own, axis, halves):
    count = lax.axis_size(axis)
    far = count // 2
    mid = own.shape[0] // 2
    found = [(0, 0, own)]
    low, high = own, own
    for k in range(1, far):
        low, high = turned(low, axis, 1), turned(high, axis, -1)
        found += [(count - k, 0, low), (k, 0, high)]
    if not halves:
        return found + [(far, 0, turned(low, axis, 1))]
    last = [(far, 0, turned(low[:mid], axis, 1)), (far, mid, turned(high[mid:], axis, -1))]
    return found + last


def direct(own, axis):
    return [
        (0, 0, own),
        (3, 0, turned(own, axis, 1)),
        (1, 0, turned(own, axis, -1)),
        (2, 0, turned(own, axis, 2)),
    ]


def in_hbm(value):
    return pltpu.with_memory_space_constraint(value, pltpu.HBM)


def run_copies(copies):
    for c in copies:
        c.start()
    for c in copies:
        c.wait()


def joined(found, axis):
    rows, cols = found[0][2].shape
    count = len(found)

    def body(place, *refs):
        out, sems = refs[count:]
        run_copies(
            [
                pltpu.make_async_copy(
                    refs[n], out.at[pl.ds((place[0] + found[n][0]) % count * rows, rows)], sems.at[n]
                )
                for n in range(count)
            ]
        )

    return pl.pallas_call(
        body,
        in_specs=[SMEM] + [HBM] * count,
        out_specs=VMEM,
        out_shape=jax.ShapeDtypeStruct((count * rows, cols), BF),
        scratch_shapes=[pltpu.SemaphoreType.DMA((count,))],
    )(lax.axis_index(axis).astype(jnp.int32)[None], *(b for _, _, b in found))


def narrowed(l, up, gate, down):
    rows, hid = up.shape[1:]
    mid = rows // 2

    def body(*refs):
        for k, source in enumerate(refs[:3]):
            for half, out in enumerate(refs[3:]):
                out[:, k * hid : (k + 1) * hid] = source[0, half * mid : (half + 1) * mid].astype(BF)

    spec = pl.BlockSpec((1, rows, hid), lambda i: (l, 0, 0))
    out = pl.BlockSpec((mid, 3 * hid), lambda i: (0, 0))
    return pl.pallas_call(
        body,
        grid=(1,),
        in_specs=[spec] * 3,
        out_specs=[out] * 2,
        out_shape=[jax.ShapeDtypeStruct((mid, 3 * hid), BF)] * 2,
    )(up, gate, down)


def weight_copy(place, kind, ref, w, q, sem):
    half, axis, distance, first = kind
    z, y, x, c = (place[k] for k in range(4))
    cols = w.shape[1]
    slots = w.reshape(NC, NX, NZ, NY, 8, cols)
    cb = half * 4 + q
    core = (cb % 2 + c) % 2
    column = (cb // 2 - x + NX) % NX
    if axis == "y":
        source = ref.reshape(NZ, 4, 8, cols).at[:, q]
        target = slots.at[core, column, :, (y + distance) % NY]
    elif axis == "z":
        count = ref.shape[0] // 32
        source = ref.reshape(count, 4, 8, cols).at[:, q]
        target = slots.at[core, column, (z + distance) % NZ, pl.ds(first // 32, count)]
    else:
        source = ref.reshape(NZ, NY, 4, 8, cols).at[:, :, q]
        target = slots.at[core, column]
    return pltpu.make_async_copy(source, target, sem)


def products(place, state, gain, plan, pieces, scale):
    span = state[0].shape[-1]
    wide = scale.shape[0]
    half = state[0].shape[0]
    block = half // NX
    cols = pieces[0].shape[1]
    chunk = 256

    def body(place, near, other, gains, scales, *refs):
        pieces, (out, w, scaled, column, sems) = refs[: len(plan)], refs[len(plan) :]

        @pl.loop(0, 4)
        def _(q):
            for n, kind in enumerate(plan):
                weight_copy(place, kind, pieces[n], w, q, sems.at[n * 4 + q]).start()

        @pl.loop(0, 2 * half // 128)
        def _(r):
            lanes = jnp.broadcast_to(gains[pl.ds(r, 1), :], (8, 128))
            column[pl.ds(r * 16, 16)] = jnp.transpose(lanes)[:, :1].reshape(16, 8, 1)

        squares = jnp.zeros((1, span), F32)
        for k, source in enumerate((near, other)):

            def scale_block(m, squares):
                values = source[pl.ds(m * block, block)].astype(F32)
                cb = (place[2] + m) % NX * 2 + (place[3] + k) % 2
                own = column.reshape(NZ * NY, 8, 8, 1)[:, pl.ds(cb, 1)].reshape(block, 1)
                scaled[pl.ds(k * half + m * block, block), :] = (values * own).astype(BF)
                return squares + jnp.sum(values * values, axis=0, keepdims=True)

            squares = lax.fori_loop(0, NX, scale_block, squares)
        inverse = lax.rsqrt(squares / (2 * half) + EPS)
        inverse = jnp.transpose(jnp.broadcast_to(inverse, (8, span)))[:, :1]

        @pl.loop(0, 4)
        def _(q):
            for n, kind in enumerate(plan):
                weight_copy(place, kind, pieces[n], w, q, sems.at[n * 4 + q]).wait()

        @pl.loop(0, wide // chunk)
        def _(n):
            at = pl.ds(pl.multiple_of(n * chunk, chunk), chunk)
            raw = lax.dot_general(
                scaled[...], w[:, at], (((0,), (0,)), ((), ())), preferred_element_type=F32
            )
            out[:, at] = raw * inverse * scales[:, at]

    return pl.pallas_call(
        body,
        in_specs=[SMEM] + [VMEM] * 4 + [HBM] * len(plan),
        out_specs=[VMEM] * 2,
        out_shape=[
            jax.ShapeDtypeStruct((span, wide), F32),
            jax.ShapeDtypeStruct((2 * half, cols), BF),
        ],
        scratch_shapes=[
            pltpu.VMEM((2 * half, span), BF),
            pltpu.VMEM((2 * half // 8, 8, 1), F32),
            pltpu.SemaphoreType.DMA((4 * len(plan),)),
        ],
        compiler_params=pltpu.CompilerParams(vmem_limit_bytes=24 << 20),
    )(place, *state, gain, scale[None], *map(in_hbm, pieces))


def down_of(hidden, w):
    span, hid = hidden.shape
    half = w.shape[0] // 2
    first = w.shape[1] - hid

    def body(hidden, w, kept, sent):
        for k, out in ((1, sent), (0, kept)):
            out[...] = lax.dot_general(
                w[k * half : (k + 1) * half, first:],
                hidden[...],
                (((1,), (1,)), ((), ())),
                preferred_element_type=F32,
            ).astype(BF)

    return pl.pallas_call(
        body,
        in_specs=[VMEM] * 2,
        out_specs=[VMEM] * 2,
        out_shape=[jax.ShapeDtypeStruct((half, span), BF)] * 2,
        compiler_params=pltpu.CompilerParams(vmem_limit_bytes=16 << 20),
    )(hidden, w)


def gather_cb(own):
    found = sorted(direct(own, "x"), key=lambda f: f[0])
    near = jnp.concatenate([b for _, _, b in found], axis=0)
    return near, turned(near, "c", 1)


def scatter_cb(kept, sent):
    got = turned(sent, "c", 1)
    rows = kept.shape[0] // NX

    def pair(k):
        at = slice(k * rows, (k + 1) * rows)
        return kept[at].astype(F32) + got[at].astype(F32)

    sums = [turned(pair(k).astype(BF), "x", k) for k in (1, 3, 2)]
    total = pair(0)
    for s in sums:
        total = total + s.astype(F32)
    return total


def taps_of(values, before, taps):
    edge = before.shape[0]
    rows = jnp.concatenate([before, values], axis=0)
    total = taps[edge][None, :] * values
    for k in range(edge):
        total = total + taps[k][None, :] * rows[k : k + values.shape[0]]
    return total


def per_device(
    tokens,
    norm_gain,
    up_weight,
    gate_weight,
    up_scale,
    gate_scale,
    up_taps,
    gate_taps,
    down_weight,
    down_scale,
):
    rows, hid = up_weight.shape[1:]
    ra = lax.axis_size(RA)
    z, y, x, c = (lax.axis_index(a) for a in ("z", "y", "x", "c"))
    place = jnp.stack([z, y, x, c]).astype(jnp.int32)
    cb = x * 2 + c
    part = rows // 8
    span = tokens.shape[1] // ra
    block = part * ra

    own_a, own_b = narrowed(0, up_weight, gate_weight, down_weight)
    by_z_a = ring(own_a, "z", False)
    y_b = joined(direct(own_b, "y"), "y")
    by_z = ring(y_b, "z", False)
    z_a = joined(by_z_a, "z")
    by_y = direct(z_a, "y")
    plan0 = [(0, "y", d, r) for d, r, _ in by_y] + [(1, "z", d, r) for d, r, _ in by_z]
    w0 = [b for *_, b in by_y] + [b for *_, b in by_z]

    own_a2, own_b2 = narrowed(1, up_weight, gate_weight, down_weight)
    z_a2 = lax.all_gather(after(own_a2, by_z_a[-1][2]), "z", axis=0, tiled=True)
    y_b2 = joined(direct(own_b2, "y"), "y")
    by_y2 = direct(after(z_a2, by_y[-1][2], by_y[-2][2]), "y")

    own = lax.dynamic_slice_in_dim(tokens, cb * part, part, 0)
    own = own.reshape(part, ra, span).transpose(1, 0, 2)
    none = jnp.zeros((1, part, AHEAD), BF)
    before = jnp.concatenate([none, own[:-1, :, span - AHEAD :]], axis=0)
    own = jnp.concatenate([before, own], axis=2)
    own = lax.all_to_all(own, RA, split_axis=0, concat_axis=0, tiled=True)
    scales = lax.dynamic_index_in_dim(down_scale.reshape(2, ra, 8, part), cb, 2, keepdims=False)
    own, scales = lax.optimization_barrier((own.reshape(block, AHEAD + span), scales.reshape(2, block, 1)))
    state = gather_cb(own)
    w1_b = lax.all_gather(after(y_b2, by_z[5][2], state[1]), "z", axis=0, tiled=True)
    plan1 = [(0, "y", d, r) for d, r, _ in by_y2] + [(1, "all", 0, 0)]
    w1 = [b for *_, b in by_y2] + [w1_b]
    state = after(state, z_a2)
    edge = up_taps.shape[1] - 1

    for l, plan, w in ((0, plan0, w0), (1, plan1, w1)):
        scale = jnp.concatenate([up_scale[l], gate_scale[l]])
        pre, rows_w = products(place, state, norm_gain[l].reshape(-1, 128), plan, w, scale)
        if l == 0:
            before, pre, own = pre[AHEAD - edge : AHEAD], pre[AHEAD:], own[:, AHEAD:]
        else:
            before = shifted(pre[-edge:], RA, 1)
        conv_up = taps_of(pre[:, :hid], before[:, :hid], up_taps[l])
        conv_gate = taps_of(pre[:, hid:], before[:, hid:], gate_taps[l])
        hidden = (jax.nn.silu(conv_gate) * conv_up).astype(BF)
        sums = scatter_cb(*down_of(hidden, rows_w))
        own = (sums * scales[l] + RESIDUAL * own.astype(F32)).astype(BF)
        if l == 0:
            state = gather_cb(own)

    piece = own.reshape(ra, part, span)
    piece = lax.all_to_all(piece, RA, split_axis=0, concat_axis=0, tiled=True)
    piece = piece.transpose(1, 0, 2).reshape(part, ra * span)
    whole = jnp.zeros((NX, part, ra * span), BF)
    for distance, _, found in direct(piece, "x"):
        whole = lax.dynamic_update_index_in_dim(whole, found, (x + distance) % NX, 0)
    other = turned(whole, "c", 1)
    even = jnp.where(c == 0, whole, other)
    odd = jnp.where(c == 0, other, whole)
    return jnp.stack([even, odd], axis=1).reshape(rows, ra * span)


def solution(mesh):
    torus = Mesh(mesh.devices.reshape(NZ, NY, NX, NC), ("z", "y", "x", "c"))
    placed = (
        P(RA, None),
        P(),
        P(None, RA, CB),
        P(None, RA, CB),
        P(None, CB),
        P(None, CB),
        P(None, None, CB),
        P(None, None, CB),
        P(None, RA, CB),
        P(),
    )

    return jax.shard_map(per_device, mesh=torus, in_specs=placed, out_specs=P(RA, None), check_vma=False)
```
